128 devices in a mesh: sp: 64 (over z, y, x), tp: 2 (over core).
Axes of the slice: x: 4, y: 4, z: 4, core: 2. Of those that a mesh axis runs over, the one named last changes fastest.
Arguments:
- residual: bfloat16 [16384, 2048], P(('sp', 'tp')), as said below
- outer_gate: bfloat16 [16384, 1024], P('sp', 'tp'), may hold values from -6 to 6
- conv_input: bfloat16 [16384, 1024], P('sp', 'tp'), as said below
- conv_value: bfloat16 [16384, 1024], P('sp', 'tp'), may hold values from -6 to 6
- doc_ids: int32 [16384], P('sp'), may hold values from 0 to 31, never falling along the last dimension, each value on 1 to 1024 neighbouring positions
- conv_taps: bfloat16 [3, 1024], P(None, 'tp'), may hold values from -3.5 to 3.5
- branch_gain: bfloat16 [1024], P('tp'), may hold values from 0.099609375 to 1.8984375
- out_weight: bfloat16 [1024, 2048], replicated, may hold values from -0.1875 to 0.1875
- ffn_gain: bfloat16 [2048], replicated, may hold values from 0.099609375 to 1.8984375
- route_ids: int32 [16384, 4], P(('sp', 'tp')), may hold values from 0 to 127, all different within a row; in each aligned block of 128 rows (0 to 127, 128 to 255, ...) at most 8 rows name the same one
- route_weight: float32 [16384, 4], P(('sp', 'tp')), may hold values from 0.2 to 1
- shared_gate: bfloat16 [2048, 512], replicated, may hold values from -0.125 to 0.125
- shared_up: bfloat16 [2048, 512], replicated, may hold values from -0.125 to 0.125
- shared_down: bfloat16 [512, 2048], replicated, may hold values from -0.25 to 0.25
- expert_gate: bfloat16 [128, 2048, 512], P(('sp', 'tp')), may hold values from -0.125 to 0.125
- expert_up: bfloat16 [128, 2048, 512], P(('sp', 'tp')), may hold values from -0.125 to 0.125
- expert_down: bfloat16 [128, 512, 2048], P(('sp', 'tp')), may hold values from -0.25 to 0.25
Outputs:
- layer_out: bfloat16 [16384, 2048], P(('sp', 'tp'))
The draws below stay inside these ranges and needn't reach their ends.
Inputs may be any that keep to these rules, and one draw needn't show every extreme that they name: `route_ids`: each row names 4 different experts. Within each aligned block of 128 rows (the rows of one device) no expert is named by more than 8 rows, and in every draw some expert is named by exactly 8 rows of some block. `doc_ids`: document numbers start at 0 and never fall along the sequence; each document has 1 to 1024 positions. `residual`: Real-valued, of order one. `conv_input`: Real-valued, of order one.
All inputs are finite; a program needn't handle non-finite values.
Results may differ from the reference program's by a relative error of at most 0.012.
Values may be sent and summed in bfloat16 or wider, within the bound.
No kernel may reach another device: no remote copies, remote signals or barrier semaphores. Data moves between devices by JAX's collectives and lax.ppermute only.
A program may use at most 128 MiB of HBM per device.

```python
import math
import jax
import jax.numpy as jnp
import numpy as np
from jax import lax

D = 2048
CH = 1024
EFF = 512
SFF = 512
TAPS = 3
TOP = 4
TOK_DEV = 256
TOKENS = 16384
ROWS_DEV = 128
EXPERTS = 128
CAP = 8
DOCS = 32
N_TP = 2


def draw_residual(key, part):
    keys = jax.random.split(key, 2)
    base = jax.random.normal(keys[0], (TOKENS, D), jnp.float32)
    column_scale = jnp.exp(jax.random.uniform(keys[1], (1, D), jnp.float32, math.log(0.4), math.log(2.5)))
    values = base * column_scale
    return values.astype(jnp.bfloat16)


def draw_conv_input(key, part):
    keys = jax.random.split(key, 2)
    rising = jnp.exp(jnp.linspace(math.log(0.5), math.log(2.0), CH))[None, :]
    jitter = jax.random.uniform(keys[1], (1, CH), jnp.float32, 0.7, 1.4)
    base = jax.random.normal(keys[0], (TOKENS, CH), jnp.float32)
    values = base * rising * jitter
    return values.astype(jnp.bfloat16)


def shard_levels(stream_key, extent, shards, low, high):
    factor_of, own = 1.0, jax.random.fold_in(stream_key, 6)
    for dim, shards_of in shards:
        draws = jnp.exp(jax.random.uniform(jax.random.fold_in(own, dim), (shards_of,), jnp.float32, low / len(shards), high / len(shards)))
        factor_of = factor_of * jnp.repeat(draws, extent[dim] // shards_of).reshape([-1 if axis == dim else 1 for axis in range(len(extent))])
    return factor_of


def profile(number_of, total, most, lean):
    weights = [(1 << 20) // math.isqrt(standing ** lean) + 1 for standing in range(2, number_of + 1)]
    surplus, holding = total - most - (number_of - 1), [1] * (number_of - 1)
    while surplus > 0:
        movable = [i for i in range(number_of - 1) if holding[i] < most]
        mass, left = sum([weights[i] for i in movable]), surplus
        for i in movable:
            addition = min(most - holding[i], max(1, left * weights[i] // mass), surplus)
            holding[i] = holding[i] + addition
            surplus = surplus - addition
    return np.array([most] + holding)


def ragged_sizes(stream_key, number_of, total, bound, slope):
    if number_of == 2:
        one = jax.random.randint(stream_key, (), max(1, total - bound), min(bound, total - 1) + 1)
        return jnp.stack([one, total - one])
    tallies = jnp.asarray(profile(number_of, total, bound, slope), jnp.int32)
    pairs = (number_of - 1) // 2
    source_of, receiver = tallies[1:1 + 2 * pairs:2], tallies[2:2 + 2 * pairs:2]
    margin = jnp.minimum(source_of - 1, bound - receiver)
    shifted = jax.random.randint(jax.random.fold_in(stream_key, 1), (pairs,), 0, 1 << 20) % (margin + 1)
    tallies = tallies.at[1:1 + 2 * pairs:2].set(source_of - shifted).at[2:2 + 2 * pairs:2].set(receiver + shifted)
    return tallies[jax.random.permutation(jax.random.fold_in(stream_key, 2), number_of)]


def routed_block(stream_key, own, number, rows, number_of, top, bound, skew):
    order = jax.random.permutation(stream_key, number_of)
    heavy_load, usual = load_shares(number_of, rows * top, bound, skew, True), load_shares(number_of, rows * top, bound, skew, False)
    places = jnp.arange(number_of)

    def named(tallies, offset_by):
        used = int((tallies > 0).sum())
        fixed = max(1, used // 4)
        shifted = fixed + (places - fixed + offset_by * (used - fixed)) % max(1, number_of - fixed)
        return jnp.zeros((number_of,), jnp.int32).at[order[jnp.where(places < fixed, places, shifted)]].set(jnp.asarray(tallies, jnp.int32))

    tallies = jnp.where(number % 4 == 0, named(heavy_load, number // 4), named(usual, number - number // 4 - 1))
    mixed = jax.random.permutation(jax.random.fold_in(own, 3), number_of)
    donor, taker = mixed[0:number_of // 2 * 2:2], mixed[1:number_of // 2 * 2:2]
    margin = jnp.minimum(tallies[donor] - 1, bound - tallies[taker]) // 2
    margin = jnp.where((donor == order[0]) | (taker == order[0]) | (tallies[taker] == 0), 0, jnp.maximum(margin, 0))
    shifted = jax.random.randint(jax.random.fold_in(own, 4), (number_of // 2,), 0, 1 << 20) % (margin + 1)
    tallies = tallies.at[donor].add(-shifted).at[taker].add(shifted)
    items = jnp.searchsorted(jnp.cumsum(tallies), jnp.arange(rows * top), side="right").astype(jnp.int32)
    grid = items.reshape(top, rows).T
    grid = grid[jax.random.permutation(jax.random.fold_in(own, 1), rows)]
    offset_by = jax.random.randint(jax.random.fold_in(own, 2), (rows, 1), 0, top)
    return jnp.take_along_axis(grid, (jnp.arange(top)[None, :] + offset_by) % top, axis=1)


def load_shares(number_of, total, reach, skew, full):
    portions = [(1 << 20) // math.isqrt(grade ** skew) + 1 for grade in range(1, number_of + 1)]
    largest = reach if full else min(reach, max(-(-total // number_of), total * portions[0] // sum(portions)))
    least = 1 if total - largest >= number_of - 1 else 0
    holding, spare = [largest] + [least] * (number_of - 1), total - largest - least * (number_of - 1)
    while spare > 0:
        candidates = [i for i in range(1, number_of) if holding[i] < largest] or [i for i in range(1, number_of) if holding[i] < reach]
        pool, budget = sum([portions[i] for i in candidates]), spare
        for i in candidates:
            addition = min(reach - holding[i], max(1, budget * portions[i] // pool), spare)
            holding[i] = holding[i] + addition
            spare = spare - addition
    return np.array(holding)


def bell_draw(key, shape, scale, bound, cuts=(), kind=jnp.bfloat16):
    values = scale * jax.random.normal(key, shape, jnp.float32)
    if cuts:
        values = values * shard_levels(key, shape, cuts, -0.22, 0.18)
    return jnp.clip(values, -bound, bound).astype(kind)


def setup_inputs(seed: int = 0) -> dict:
    streams_of = jax.random.split(jax.random.key(seed), 18)
    residual = draw_residual(jax.random.fold_in(streams_of[17], 71), 0)
    outer_gate = bell_draw(streams_of[1], (TOKENS, CH), 1.0, 6.0, ((0, 64), (1, 2)))
    conv_input = draw_conv_input(jax.random.fold_in(streams_of[17], 71), 0)
    conv_value = bell_draw(streams_of[3], (TOKENS, CH), 1.0, 6.0, ((0, 64), (1, 2)))
    doc_ids = jnp.searchsorted(jnp.cumsum(ragged_sizes(streams_of[4], DOCS, TOKENS, 4 * TOK_DEV, 1)), jnp.arange(TOKENS), side="right").astype(jnp.int32)
    conv_taps = bell_draw(streams_of[5], (TAPS, CH), TAPS ** -0.5, 3.5, ((1, 2),))
    branch_gain = jnp.clip(1.0 + 0.18 * jax.random.normal(streams_of[6], (CH,), jnp.float32), 0.099609375, 1.8984375).astype(jnp.bfloat16)
    out_weight = bell_draw(streams_of[7], (CH, D), CH ** -0.5, 0.1875)
    ffn_gain = jnp.clip(1.0 + 0.18 * jax.random.normal(streams_of[8], (D,), jnp.float32), 0.099609375, 1.8984375).astype(jnp.bfloat16)
    route_ids_keys = jax.random.split(jax.random.fold_in(streams_of[9], 1), TOKENS // ROWS_DEV)
    route_ids_turns = jax.random.permutation(jax.random.fold_in(streams_of[9], 3), TOKENS // ROWS_DEV)
    route_ids = jax.vmap(lambda own, number: routed_block(jax.random.fold_in(streams_of[9], 2), own, number, ROWS_DEV, EXPERTS, TOP, CAP, 2))(route_ids_keys, route_ids_turns).reshape((TOKENS, TOP))
    route_weight = jnp.clip(0.2 + 0.8 * jax.random.uniform(streams_of[10], (TOKENS, TOP), jnp.float32) ** shard_levels(streams_of[10], (TOKENS, TOP), ((0, 128),), -0.2, 0.2), 0.2, 1.0)
    shared_gate = bell_draw(streams_of[11], (D, SFF), D ** -0.5, 0.125)
    shared_up = bell_draw(streams_of[12], (D, SFF), D ** -0.5, 0.125)
    shared_down = bell_draw(streams_of[13], (SFF, D), SFF ** -0.5, 0.25)
    expert_gate = bell_draw(streams_of[14], (EXPERTS, D, EFF), D ** -0.5, 0.125, ((0, 128),))
    expert_up = bell_draw(streams_of[15], (EXPERTS, D, EFF), D ** -0.5, 0.125, ((0, 128),))
    expert_down = bell_draw(streams_of[16], (EXPERTS, EFF, D), EFF ** -0.5, 0.25, ((0, 128),))
    return dict(residual=residual, outer_gate=outer_gate, conv_input=conv_input, conv_value=conv_value, doc_ids=doc_ids, conv_taps=conv_taps, branch_gain=branch_gain, out_weight=out_weight, ffn_gain=ffn_gain, route_ids=route_ids, route_weight=route_weight, shared_gate=shared_gate, shared_up=shared_up, shared_down=shared_down, expert_gate=expert_gate, expert_up=expert_up, expert_down=expert_down)


norm_eps = 1e-06

def reference(residual, outer_gate, conv_input, conv_value, doc_ids, conv_taps, branch_gain, out_weight, ffn_gain, route_ids, route_weight, shared_gate, shared_up, shared_down, expert_gate, expert_up, expert_down):
    source = conv_input.astype(jnp.float32) * conv_value.astype(jnp.float32)
    mixed_conv = jnp.zeros(source.shape, jnp.float32)
    for tap in range(TAPS):
        tap_lag = TAPS - 1 - tap
        lagged = jnp.pad(source, ((tap_lag, 0), (0, 0)))[:TOKENS]
        lagged_doc = jnp.pad(doc_ids, (tap_lag, 0), constant_values=-1)[:TOKENS]
        same_doc = (lagged_doc == doc_ids).astype(jnp.float32)[:, None]
        mixed_conv = mixed_conv + conv_taps[tap].astype(jnp.float32)[None, :] * lagged * same_doc
    branch = outer_gate.astype(jnp.float32) * mixed_conv
    inv_rms = lax.rsqrt(lax.optimization_barrier(jnp.mean(branch * branch, axis=1, keepdims=True)) + norm_eps)
    normed = (branch * inv_rms * branch_gain.astype(jnp.float32)[None, :]).astype(jnp.bfloat16)
    update = jnp.dot(normed, out_weight, preferred_element_type=jnp.float32)
    middle = (residual.astype(jnp.float32) + update).astype(jnp.bfloat16)
    mid_float = middle.astype(jnp.float32)
    mid_rms = lax.rsqrt(lax.optimization_barrier(jnp.mean(mid_float * mid_float, axis=1, keepdims=True)) + norm_eps)
    ffn_in = (mid_float * mid_rms * ffn_gain.astype(jnp.float32)[None, :]).astype(jnp.bfloat16)
    shared_hidden = (jax.nn.silu(jnp.dot(ffn_in, shared_gate, preferred_element_type=jnp.float32)) * jnp.dot(ffn_in, shared_up, preferred_element_type=jnp.float32)).astype(jnp.bfloat16)
    shared_out = jnp.dot(shared_hidden, shared_down, preferred_element_type=jnp.float32)
    block_rows = TOK_DEV // N_TP
    block_count = TOKENS // block_rows
    flat_expert = route_ids.reshape(block_count, block_rows * TOP)
    onehot = (flat_expert[:, :, None] == jnp.arange(EXPERTS, dtype=jnp.int32)[None, None, :]).astype(jnp.int32)
    slot_rank = lax.optimization_barrier(jnp.sum(onehot * (jnp.cumsum(onehot, axis=1) - onehot), axis=2))
    block_index = jnp.arange(block_count, dtype=jnp.int32)[:, None]
    slot_index = (flat_expert * (block_count * CAP) + block_index * CAP + slot_rank).reshape(-1)
    token_index = (jnp.arange(TOKENS * TOP, dtype=jnp.int32) // TOP).astype(jnp.int32)
    slot_token = jnp.full((EXPERTS * block_count * CAP,), TOKENS, jnp.int32).at[slot_index].set(token_index)
    slot_weight = jnp.zeros((EXPERTS * block_count * CAP,), jnp.float32).at[slot_index].set(route_weight.reshape(-1))
    slot_token = slot_token.reshape(EXPERTS, block_count * CAP)
    slot_weight = slot_weight.reshape(EXPERTS, block_count * CAP)
    padded_in = jnp.concatenate([ffn_in, jnp.zeros((1, D), jnp.bfloat16)], axis=0)

    def one_expert(total_sum, inputs):
        tokens_here, weights_here, gate_w, up_w, down_w = inputs
        gathered = padded_in[tokens_here]
        hidden = (jax.nn.silu(jnp.dot(gathered, gate_w, preferred_element_type=jnp.float32)) * jnp.dot(gathered, up_w, preferred_element_type=jnp.float32)).astype(jnp.bfloat16)
        result = jnp.dot(hidden, down_w, preferred_element_type=jnp.float32).astype(jnp.bfloat16)
        total_sum = total_sum.at[tokens_here].add(result.astype(jnp.float32) * weights_here[:, None])
        return (total_sum, None)
    routed, _ = lax.scan(one_expert, jnp.zeros((TOKENS + 1, D), jnp.float32), (slot_token, slot_weight, expert_gate, expert_up, expert_down))
    return (mid_float + shared_out + routed[:TOKENS]).astype(jnp.bfloat16)
```

```python
import functools
import jax
import jax.numpy as jnp
from jax import lax
from jax.experimental import pallas as pl
from jax.experimental.pallas import tpu as pltpu
from jax.sharding import PartitionSpec as P

norm_eps = 1e-06
BF = jnp.bfloat16
F32 = jnp.float32
MIB = 1 << 20
LANES = 128

VM = pl.BlockSpec(memory_space=pltpu.VMEM)
SM = pl.BlockSpec(memory_space=pltpu.SMEM)
ANY = pl.BlockSpec(memory_space=pl.ANY)


def params(mib):
    return pltpu.CompilerParams(vmem_limit_bytes=mib * MIB)


def cost(flops, nbytes):
    return pl.CostEstimate(flops=flops, bytes_accessed=nbytes, transcendentals=0)


def dot(a, b):
    return jnp.dot(a, b, preferred_element_type=F32)


def slots_kernel(ids_ref, out_ref, *, capacity):
    slots, rows = out_ref.shape
    expert = lax.broadcasted_iota(jnp.int32, (slots, rows), 0) // capacity
    place = lax.broadcasted_iota(jnp.int32, (slots, rows), 0) % capacity
    named = expert == ids_ref[0:1, :]
    for k in range(1, ids_ref.shape[0]):
        named = jnp.logical_or(named, expert == ids_ref[k : k + 1, :])
    hit = named.astype(F32)
    before = lax.broadcasted_iota(jnp.int32, (rows, rows), 0) < lax.broadcasted_iota(
        jnp.int32, (rows, rows), 1
    )
    rank = dot(hit.astype(BF), before.astype(F32).astype(BF))
    out_ref[...] = jnp.where(rank == place.astype(F32), hit, 0.0).astype(BF)


def conv_kernel(
    half_ref, gate_ref, input_ref, value_ref, doc_ref, halo_ref, taps_ref, gain_ref,
    own_ref, send_ref, ext_ref, all_ref,
):
    rows, width = gate_ref.shape
    taps = taps_ref.shape[0]
    lead = taps - 1
    doc = jnp.transpose(jnp.broadcast_to(doc_ref[...].astype(F32), (LANES, rows)))
    ext_ref[8:, :width] = input_ref[...].astype(F32) * value_ref[...].astype(F32)
    ext_ref[8:, width:] = doc
    halo = halo_ref[...].astype(F32)
    ext_ref[8 - lead : 8, :width] = halo[0:lead] * halo[lead : 2 * lead]
    ext_ref[8 - lead : 8, width:] = halo[2 * lead : 3 * lead, :LANES]
    mixed = jnp.zeros((rows, width), F32)
    for tap in range(taps):
        start = 8 - lead + tap
        same = (ext_ref[start : start + rows, width:] == doc).astype(F32)
        same = jnp.concatenate([same] * (width // LANES), axis=1)
        mixed = mixed + taps_ref[tap : tap + 1, :].astype(F32) * ext_ref[start : start + rows, :width] * same
    branch = gate_ref[...].astype(F32) * mixed
    total = jnp.broadcast_to(jnp.sum(branch * branch, axis=1, keepdims=True), (rows, LANES))
    high = total.astype(BF).astype(F32)
    middle = (total - high).astype(BF).astype(F32)
    low = total - high - middle
    part = lax.broadcasted_iota(jnp.int32, (rows, LANES), 1) % 4
    packed = jnp.where(part == 0, high, jnp.where(part == 1, middle, jnp.where(part == 2, low, 0.0)))
    all_ref[:, :width] = branch * gain_ref[...].astype(F32)
    all_ref[:, width:] = packed
    half = half_ref[0]
    local = rows // 2
    own_ref[...] = all_ref[pl.ds(pl.multiple_of(half * local, local), local), :].astype(BF)
    send_ref[...] = all_ref[pl.ds(pl.multiple_of((1 - half) * local, local), local), :].astype(BF)


def mid_kernel(
    half_ref, own_ref, recv_ref, weight_ref, residual_ref, gain_ref, slots_ref,
    mid_ref, ffn_ref, out_ref, buf_ref, sems, *, chunks,
):
    width = weight_ref.shape[0] // 2
    half = half_ref[0]
    squares = jnp.sum(
        own_ref[:, width:].astype(F32) + recv_ref[:, width:].astype(F32), axis=1, keepdims=True
    ) * (4.0 / LANES)
    inv_rms = lax.rsqrt(squares / (2 * width) + norm_eps)
    update = dot(own_ref[:, :width], weight_ref[pl.ds(pl.multiple_of(half * width, width), width), :])
    update = update + dot(
        recv_ref[:, :width], weight_ref[pl.ds(pl.multiple_of((1 - half) * width, width), width), :]
    )
    mid = (residual_ref[...].astype(F32) + update * inv_rms).astype(BF)
    mid_ref[...] = mid
    mid_float = mid.astype(F32)
    mid_rms = lax.rsqrt(jnp.mean(mid_float * mid_float, axis=1, keepdims=True) + norm_eps)
    ffn = (mid_float * mid_rms * gain_ref[...].astype(F32)).astype(BF)
    ffn_ref[...] = ffn
    step = slots_ref.shape[0] // chunks
    copies = []
    for i in range(chunks):
        at = pl.ds(i * step, step)
        buf_ref[at, :] = dot(slots_ref[at, :], ffn).astype(BF)
        copies.append(pltpu.make_async_copy(buf_ref.at[at, :], out_ref.at[at, :], sems.at[i]))
        copies[-1].start()
    for copy in copies:
        copy.wait()


def expert_kernel(x_ref, gate_ref, up_ref, down_ref, out_ref, buf_ref, sems, *, chunks):
    step = x_ref.shape[0] // chunks
    copies = []
    for i in range(chunks):
        at = pl.ds(i * step, step)
        rows = x_ref[at, :]
        hidden = (jax.nn.silu(dot(rows, gate_ref[...])) * dot(rows, up_ref[...])).astype(BF)
        buf_ref[at, :] = dot(hidden, down_ref[...]).astype(BF)
        copies.append(pltpu.make_async_copy(buf_ref.at[at, :], out_ref.at[at, :], sems.at[i]))
        copies[-1].start()
    for copy in copies:
        copy.wait()


def shared_kernel(
    ffn_ref, mid_ref, gate_ref, up_ref, down_ref, ids_ref, share_ref, base_ref, mix_ref, *, capacity
):
    ffn = ffn_ref[...]
    hidden = (jax.nn.silu(dot(ffn, gate_ref[...])) * dot(ffn, up_ref[...])).astype(BF)
    base_ref[...] = mid_ref[...].astype(F32) + dot(hidden, down_ref[...])
    rows = ids_ref.shape[0]
    slots = mix_ref.shape[1]
    lane = lax.broadcasted_iota(jnp.int32, (rows, slots), 1)
    expert = lane // capacity
    place = (lane % capacity).astype(F32)
    hit = jnp.zeros((rows, slots), F32)
    share = jnp.zeros((rows, slots), F32)
    for k in range(ids_ref.shape[1]):
        named = expert == ids_ref[:, k : k + 1]
        hit = jnp.where(named, 1.0, hit)
        share = jnp.where(named, share_ref[:, k : k + 1], share)
    before = lax.broadcasted_iota(jnp.int32, (rows, rows), 1) < lax.broadcasted_iota(
        jnp.int32, (rows, rows), 0
    )
    rank = dot(before.astype(F32).astype(BF), hit.astype(BF))
    share = jnp.where(rank == place, share, 0.0)
    high = share.astype(BF)
    mix_ref[:rows, :] = high
    mix_ref[rows:, :] = (share - high.astype(F32)).astype(BF)


def combine_kernel(mix_ref, base_ref, back_ref, out_ref):
    rows = out_ref.shape[0]
    both = dot(mix_ref[...], back_ref[...])
    out_ref[...] = (base_ref[...] + (both[:rows] + both[rows:])).astype(BF)


def shards(
    residual, outer_gate, conv_input, conv_value, doc_ids, conv_taps, branch_gain, out_weight,
    ffn_gain, route_ids, route_weight, shared_gate, shared_up, shared_down,
    expert_gate, expert_up, expert_down,
):
    rows, width = conv_input.shape
    local, model = residual.shape
    top = route_ids.shape[1]
    lead = conv_taps.shape[0] - 1
    peers = lax.axis_size("sp")
    cores = lax.axis_size("tp")
    experts = peers * cores
    capacity = local * cores * top // experts
    slots = experts * capacity
    wide = width + LANES
    half = lax.axis_index("tp").astype(jnp.int32).reshape(1)

    doc_tail = jnp.broadcast_to(doc_ids[rows - lead :, None].astype(BF), (lead, width))
    tail = jnp.concatenate([conv_input[rows - lead :], conv_value[rows - lead :], doc_tail], axis=0)
    halo = lax.ppermute(tail, "sp", [(i, i + 1) for i in range(peers - 1)])

    slot_hot = pl.pallas_call(
        functools.partial(slots_kernel, capacity=capacity),
        out_shape=jax.ShapeDtypeStruct((slots, local), BF),
        in_specs=[VM], out_specs=VM, name="slots",
        compiler_params=params(8), cost_estimate=cost(2 * slots * local * local, slots * local * 2),
    )(route_ids.T)

    own, send = pl.pallas_call(
        conv_kernel,
        out_shape=[jax.ShapeDtypeStruct((local, wide), BF)] * 2,
        in_specs=[SM] + [VM] * 7, out_specs=[VM, VM], name="conv",
        scratch_shapes=[pltpu.VMEM((rows + 8, wide), F32), pltpu.VMEM((rows, wide), F32)],
        compiler_params=params(12),
    )(half, outer_gate, conv_input, conv_value, doc_ids.reshape(1, rows), halo, conv_taps, branch_gain.reshape(1, width))
    recv = lax.ppermute(send, "tp", [(0, 1), (1, 0)])

    chunks = 4
    mid, ffn, outgoing = pl.pallas_call(
        functools.partial(mid_kernel, chunks=chunks),
        out_shape=[jax.ShapeDtypeStruct((local, model), BF)] * 2 + [jax.ShapeDtypeStruct((slots, model), BF)],
        in_specs=[SM] + [VM] * 6, out_specs=[VM, VM, ANY], name="mid",
        scratch_shapes=[pltpu.VMEM((slots, model), BF), pltpu.SemaphoreType.DMA((chunks,))],
        compiler_params=params(24),
    )(half, own, recv, out_weight, residual, ffn_gain.reshape(1, model), slot_hot)

    arrived = lax.all_to_all(
        outgoing.reshape(experts, capacity, model), ("sp", "tp"), split_axis=0, concat_axis=0, tiled=True
    )
    result = pl.pallas_call(
        functools.partial(expert_kernel, chunks=chunks),
        out_shape=jax.ShapeDtypeStruct((slots, model), BF),
        in_specs=[VM] * 4, out_specs=ANY, name="expert",
        scratch_shapes=[pltpu.VMEM((slots, model), BF), pltpu.SemaphoreType.DMA((chunks,))],
        compiler_params=params(24),
    )(arrived.reshape(slots, model), expert_gate[0], expert_up[0], expert_down[0])
    result, ffn, mid = lax.optimization_barrier((result, ffn, mid))
    returned = lax.all_to_all(
        result.reshape(experts, capacity, model), ("sp", "tp"), split_axis=0, concat_axis=0, tiled=True
    ).reshape(slots, model)

    hidden = shared_gate.shape[1]
    base, mix = pl.pallas_call(
        functools.partial(shared_kernel, capacity=capacity),
        out_shape=[jax.ShapeDtypeStruct((local, model), F32), jax.ShapeDtypeStruct((2 * local, slots), BF)],
        in_specs=[VM] * 7, out_specs=[VM, VM], name="shared",
        compiler_params=params(24), cost_estimate=cost(40 * local * model * hidden, 6 * model * hidden),
    )(ffn, mid, shared_gate, shared_up, shared_down, route_ids, route_weight)

    block = model // 4
    return pl.pallas_call(
        combine_kernel,
        out_shape=jax.ShapeDtypeStruct((local, model), BF),
        grid=(model // block,), name="combine",
        in_specs=[
            pl.BlockSpec((2 * local, slots), lambda i: (0, 0)),
            pl.BlockSpec((local, block), lambda i: (0, i)),
            pl.BlockSpec((slots, block), lambda i: (0, i)),
        ],
        out_specs=pl.BlockSpec((local, block), lambda i: (0, i)),
        compiler_params=params(16),
    )(mix, base, returned)


def solution(mesh):
    placed = (
        P(("sp", "tp"), None), P("sp", "tp"), P("sp", "tp"), P("sp", "tp"), P("sp"), P(None, "tp"),
        P("tp"), P(), P(), P(("sp", "tp"), None), P(("sp", "tp"), None), P(), P(), P(),
        P(("sp", "tp"), None, None), P(("sp", "tp"), None, None), P(("sp", "tp"), None, None),
    )
    return jax.shard_map(
        shards, mesh=mesh, in_specs=placed, out_specs=P(("sp", "tp"), None), check_vma=False
    )
```

```python
import functools
import jax
import jax.numpy as jnp
from jax import lax
from jax.experimental import pallas as pl
from jax.experimental.pallas import tpu as pltpu
from jax.sharding import PartitionSpec as P

norm_eps = 1e-06
BF = jnp.bfloat16
F32 = jnp.float32
MIB = 1 << 20
LANES = 128

VM = pl.BlockSpec(memory_space=pltpu.VMEM)
SM = pl.BlockSpec(memory_space=pltpu.SMEM)
HBM = pl.BlockSpec(memory_space=pltpu.HBM)
LONG = 1 << 33


def params(mib):
    return pltpu.CompilerParams(vmem_limit_bytes=mib * MIB)


def cost(flops, nbytes):
    return pl.CostEstimate(flops=flops, bytes_accessed=nbytes, transcendentals=0)


def dot(a, b):
    return jnp.dot(a, b, preferred_element_type=F32)


def tail_kernel(input_ref, value_ref, doc_ref, tail_ref):
    width = input_ref.shape[1]
    tail_ref[0:8, :] = input_ref[8:16, :]
    tail_ref[8:16, :] = value_ref[8:16, :]
    last = jnp.transpose(jnp.broadcast_to(doc_ref[...].astype(F32), (LANES, LANES)))
    tail_ref[16:24, :] = jnp.concatenate([last[LANES - 8 :, :].astype(BF)] * (width // LANES), axis=1)


def slots_kernel(ids_ref, share_ref, hot_ref, mix_ref, *, capacity):
    slots, rows = hot_ref.shape
    slot = lax.broadcasted_iota(jnp.int32, (slots, rows), 0)
    expert = slot // capacity
    place = (slot % capacity).astype(F32)
    hit = jnp.zeros((slots, rows), F32)
    share = jnp.zeros((slots, rows), F32)
    for k in range(ids_ref.shape[0]):
        named = expert == ids_ref[k : k + 1, :]
        hit = jnp.where(named, 1.0, hit)
        share = jnp.where(named, share_ref[k : k + 1, :], share)
    before = lax.broadcasted_iota(jnp.int32, (rows, rows), 0) < lax.broadcasted_iota(
        jnp.int32, (rows, rows), 1
    )
    mine = dot(hit.astype(BF), before.astype(F32).astype(BF)) == place
    hot_ref[...] = jnp.where(mine, hit, 0.0).astype(BF)
    share = jnp.transpose(jnp.where(mine, share, 0.0))
    high = share.astype(BF)
    mix_ref[:rows, :] = high
    mix_ref[rows:, :] = (share - high.astype(F32)).astype(BF)


def conv_kernel(
    half_ref, gate_ref, input_ref, value_ref, doc_ref, halo_ref, taps_ref, gain_ref,
    own_ref, send_ref, ext_ref, all_ref,
):
    rows, width = gate_ref.shape
    taps = taps_ref.shape[0]
    doc = jnp.transpose(jnp.broadcast_to(doc_ref[...].astype(F32), (LANES, rows)))
    ext_ref[8:, :width] = input_ref[...].astype(F32) * value_ref[...].astype(F32)
    ext_ref[8:, width:] = doc
    ext_ref[0:8, :width] = halo_ref[0:8, :].astype(F32) * halo_ref[8:16, :].astype(F32)
    ext_ref[0:8, width:] = halo_ref[16:24, :LANES].astype(F32)
    mixed = jnp.zeros((rows, width), F32)
    for tap in range(taps):
        start = 9 - taps + tap
        same = (ext_ref[start : start + rows, width:] == doc).astype(F32)
        same = jnp.concatenate([same] * (width // LANES), axis=1)
        mixed = mixed + taps_ref[tap : tap + 1, :].astype(F32) * ext_ref[start : start + rows, :width] * same
    branch = gate_ref[...].astype(F32) * mixed
    total = jnp.broadcast_to(jnp.sum(branch * branch, axis=1, keepdims=True), (rows, LANES))
    high = total.astype(BF).astype(F32)
    middle = (total - high).astype(BF).astype(F32)
    low = total - high - middle
    part = lax.broadcasted_iota(jnp.int32, (rows, LANES), 1) % 4
    packed = jnp.where(part == 0, high, jnp.where(part == 1, middle, jnp.where(part == 2, low, 0.0)))
    all_ref[:, :width] = branch * gain_ref[...].astype(F32)
    all_ref[:, width:] = packed
    half = half_ref[0]
    local = rows // 2
    own_ref[...] = all_ref[pl.ds(pl.multiple_of(half * local, local), local), :].astype(BF)
    send_ref[...] = all_ref[pl.ds(pl.multiple_of((1 - half) * local, local), local), :].astype(BF)


def mid_kernel(
    half_ref, own_ref, recv_ref, weight_ref, residual_ref, gain_ref, slots_ref,
    mid_ref, ffn_ref, out_ref, *, chunks,
):
    width = weight_ref.shape[0] // 2
    half = half_ref[0]
    squares = jnp.sum(
        own_ref[:, width:].astype(F32) + recv_ref[:, width:].astype(F32), axis=1, keepdims=True
    ) * (4.0 / LANES)
    inv_rms = lax.rsqrt(squares / (2 * width) + norm_eps)
    update = dot(own_ref[:, :width], weight_ref[pl.ds(pl.multiple_of(half * width, width), width), :])
    update = update + dot(
        recv_ref[:, :width], weight_ref[pl.ds(pl.multiple_of((1 - half) * width, width), width), :]
    )
    mid = (residual_ref[...].astype(F32) + update * inv_rms).astype(BF)
    mid_ref[...] = mid
    mid_float = mid.astype(F32)
    mid_rms = lax.rsqrt(jnp.mean(mid_float * mid_float, axis=1, keepdims=True) + norm_eps)
    ffn = (mid_float * mid_rms * gain_ref[...].astype(F32)).astype(BF)
    ffn_ref[...] = ffn
    step = slots_ref.shape[0] // chunks
    for i in range(chunks):
        at = pl.ds(i * step, step)
        out_ref[at, :] = dot(slots_ref[at, :], ffn).astype(BF)


def expert_kernel(
    x_ref, gate_ref, up_ref, down_ref, ffn_ref, mid_ref, shared_gate_ref, shared_up_ref, shared_down_ref,
    out_ref, base_ref, *, chunks,
):
    def apply(rows, gate, up, down):
        hidden = (jax.nn.silu(dot(rows, gate[...])) * dot(rows, up[...])).astype(BF)
        return dot(hidden, down[...])

    shared = apply(ffn_ref[...], shared_gate_ref, shared_up_ref, shared_down_ref)
    base_ref[...] = mid_ref[...].astype(F32) + shared
    step = x_ref.shape[0] // chunks
    for i in range(chunks):
        at = pl.ds(i * step, step)
        out_ref[at, :] = apply(x_ref[at, :], gate_ref, up_ref, down_ref).astype(BF)


def combine_kernel(mix_ref, base_ref, back_ref, out_ref):
    rows = out_ref.shape[0]
    both = dot(mix_ref[...], back_ref[...])
    out_ref[...] = (base_ref[...] + (both[:rows] + both[rows:])).astype(BF)


def shards(
    residual, outer_gate, conv_input, conv_value, doc_ids, conv_taps, branch_gain, out_weight,
    ffn_gain, route_ids, route_weight, shared_gate, shared_up, shared_down,
    expert_gate, expert_up, expert_down,
):
    rows, width = conv_input.shape
    local, model = residual.shape
    top = route_ids.shape[1]
    peers = lax.axis_size("sp")
    cores = lax.axis_size("tp")
    experts = peers * cores
    capacity = local * cores * top // experts
    slots = experts * capacity
    wide = width + LANES
    half = lax.axis_index("tp").astype(jnp.int32).reshape(1)

    doc = doc_ids.reshape(1, rows)
    tail = pl.pallas_call(
        tail_kernel,
        out_shape=jax.ShapeDtypeStruct((24, width), BF),
        grid=(1,), name="tail",
        in_specs=[
            pl.BlockSpec((16, width), lambda i: (rows // 16 - 1, 0)),
            pl.BlockSpec((16, width), lambda i: (rows // 16 - 1, 0)),
            pl.BlockSpec((1, LANES), lambda i: (0, rows // LANES - 1)),
        ],
        out_specs=pl.BlockSpec((24, width), lambda i: (0, 0)),
        compiler_params=params(4), cost_estimate=cost(LONG, 0),
    )(*[pltpu.with_memory_space_constraint(a, pltpu.HBM) for a in (conv_input, conv_value, doc)])
    halo = lax.ppermute(tail, "sp", [(i, i + 1) for i in range(peers - 1)])

    own, send = pl.pallas_call(
        conv_kernel,
        out_shape=[jax.ShapeDtypeStruct((local, wide), BF)] * 2,
        in_specs=[SM] + [VM] * 7, out_specs=[VM, VM], name="conv",
        scratch_shapes=[pltpu.VMEM((rows + 8, wide), F32), pltpu.VMEM((rows, wide), F32)],
        compiler_params=params(6), cost_estimate=cost(LONG, 0),
    )(half, outer_gate, conv_input, conv_value, doc, halo, conv_taps, branch_gain.reshape(1, width))
    recv = lax.ppermute(send, "tp", [(0, 1), (1, 0)])

    slot_hot, mix = pl.pallas_call(
        functools.partial(slots_kernel, capacity=capacity),
        out_shape=[jax.ShapeDtypeStruct((slots, local), BF), jax.ShapeDtypeStruct((2 * local, slots), BF)],
        in_specs=[VM] * 2, out_specs=[VM] * 2, name="slots",
        compiler_params=params(6), cost_estimate=cost(LONG, 0),
    )(route_ids.T, route_weight.T)

    chunks = 4
    mid, ffn, outgoing = pl.pallas_call(
        functools.partial(mid_kernel, chunks=chunks),
        out_shape=[jax.ShapeDtypeStruct((local, model), BF)] * 2 + [jax.ShapeDtypeStruct((slots, model), BF)],
        in_specs=[SM] + [VM] * 6, out_specs=[VM, VM, VM], name="mid",
        compiler_params=params(12), cost_estimate=cost(LONG, 0),
    )(half, own, recv, out_weight, residual, ffn_gain.reshape(1, model), slot_hot)

    arrived = lax.all_to_all(
        outgoing.reshape(experts, capacity, model), ("sp", "tp"), split_axis=0, concat_axis=0, tiled=True
    ).reshape(slots, model)
    result, base = pl.pallas_call(
        functools.partial(expert_kernel, chunks=chunks),
        out_shape=[jax.ShapeDtypeStruct((slots, model), BF), jax.ShapeDtypeStruct((local, model), F32)],
        in_specs=[VM] * 9, out_specs=[VM] * 2, name="expert",
        compiler_params=params(12), cost_estimate=cost(LONG, 0),
    )(arrived, expert_gate[0], expert_up[0], expert_down[0], ffn, mid, shared_gate, shared_up, shared_down)
    returned = lax.all_to_all(
        result.reshape(experts, capacity, model), ("sp", "tp"), split_axis=0, concat_axis=0, tiled=True
    ).reshape(slots, model)

    return pl.pallas_call(
        combine_kernel,
        out_shape=jax.ShapeDtypeStruct((local, model), BF),
        in_specs=[VM] * 3, out_specs=VM, name="combine",
        compiler_params=params(8), cost_estimate=cost(LONG, 0),
    )(mix, base, returned)


def solution(mesh):
    placed = (
        P(("sp", "tp"), None), P("sp", "tp"), P("sp", "tp"), P("sp", "tp"), P("sp"), P(None, "tp"),
        P("tp"), P(), P(), P(("sp", "tp"), None), P(("sp", "tp"), None), P(), P(), P(),
        P(("sp", "tp"), None, None), P(("sp", "tp"), None, None), P(("sp", "tp"), None, None),
    )
    return jax.shard_map(
        shards, mesh=mesh, in_specs=placed, out_specs=P(("sp", "tp"), None), check_vma=False
    )
```

```python
import functools
import jax
import jax.numpy as jnp
from jax import lax
from jax.experimental import pallas as pl
from jax.experimental.pallas import tpu as pltpu
from jax.sharding import PartitionSpec as P

norm_eps = 1e-06
BF = jnp.bfloat16
F32 = jnp.float32
MIB = 1 << 20
LANES = 128

VM = pl.BlockSpec(memory_space=pltpu.VMEM)
SM = pl.BlockSpec(memory_space=pltpu.SMEM)
HBM = pl.BlockSpec(memory_space=pltpu.HBM)
LONG = 1 << 33
SHORT = 1 << 31


def params(mib):
    return pltpu.CompilerParams(vmem_limit_bytes=mib * MIB)


def cost(flops, nbytes):
    return pl.CostEstimate(flops=flops, bytes_accessed=nbytes, transcendentals=0)


def dot(a, b):
    return jnp.dot(a, b, preferred_element_type=F32)


def tail_kernel(input_ref, value_ref, doc_ref, tail_ref):
    width = input_ref.shape[1]
    tail_ref[0:8, :] = input_ref[8:16, :]
    tail_ref[8:16, :] = value_ref[8:16, :]
    last = jnp.transpose(jnp.broadcast_to(doc_ref[...].astype(F32), (LANES, LANES)))
    tail_ref[16:24, :] = jnp.concatenate([last[LANES - 8 :, :].astype(BF)] * (width // LANES), axis=1)


def slots_kernel(ids_ref, share_ref, hot_ref, mix_ref, *, capacity):
    slots, rows = hot_ref.shape
    slot = lax.broadcasted_iota(jnp.int32, (slots, rows), 0)
    expert = slot // capacity
    place = (slot % capacity).astype(F32)
    hit = jnp.zeros((slots, rows), F32)
    share = jnp.zeros((slots, rows), F32)
    for k in range(ids_ref.shape[0]):
        named = expert == ids_ref[k : k + 1, :]
        hit = jnp.where(named, 1.0, hit)
        share = jnp.where(named, share_ref[k : k + 1, :], share)
    before = lax.broadcasted_iota(jnp.int32, (rows, rows), 0) < lax.broadcasted_iota(
        jnp.int32, (rows, rows), 1
    )
    mine = dot(hit.astype(BF), before.astype(F32).astype(BF)) == place
    hot_ref[...] = jnp.where(mine, hit, 0.0).astype(BF)
    share = jnp.transpose(jnp.where(mine, share, 0.0))
    high = share.astype(BF)
    mix_ref[:rows, :] = high
    mix_ref[rows:, :] = (share - high.astype(F32)).astype(BF)


def conv_kernel(
    half_ref, gate_ref, input_ref, value_ref, doc_ref, halo_ref, taps_ref, gain_ref,
    own_ref, send_ref, ext_ref, all_ref,
):
    rows, width = gate_ref.shape
    taps = taps_ref.shape[0]
    doc = jnp.transpose(jnp.broadcast_to(doc_ref[...].astype(F32), (LANES, rows)))
    ext_ref[8:, :width] = input_ref[...].astype(F32) * value_ref[...].astype(F32)
    ext_ref[8:, width:] = doc
    ext_ref[0:8, :width] = halo_ref[0:8, :].astype(F32) * halo_ref[8:16, :].astype(F32)
    ext_ref[0:8, width:] = halo_ref[16:24, :LANES].astype(F32)
    mixed = jnp.zeros((rows, width), F32)
    for tap in range(taps):
        start = 9 - taps + tap
        same = (ext_ref[start : start + rows, width:] == doc).astype(F32)
        same = jnp.concatenate([same] * (width // LANES), axis=1)
        mixed = mixed + taps_ref[tap : tap + 1, :].astype(F32) * ext_ref[start : start + rows, :width] * same
    branch = gate_ref[...].astype(F32) * mixed
    total = jnp.broadcast_to(jnp.sum(branch * branch, axis=1, keepdims=True), (rows, LANES))
    high = total.astype(BF).astype(F32)
    middle = (total - high).astype(BF).astype(F32)
    low = total - high - middle
    part = lax.broadcasted_iota(jnp.int32, (rows, LANES), 1) % 4
    packed = jnp.where(part == 0, high, jnp.where(part == 1, middle, jnp.where(part == 2, low, 0.0)))
    all_ref[:, :width] = branch * gain_ref[...].astype(F32)
    all_ref[:, width:] = packed
    half = half_ref[0]
    local = rows // 2
    own_ref[...] = all_ref[pl.ds(pl.multiple_of(half * local, local), local), :].astype(BF)
    send_ref[...] = all_ref[pl.ds(pl.multiple_of((1 - half) * local, local), local), :].astype(BF)


def mid_kernel(
    half_ref, own_ref, recv_ref, weight_ref, residual_ref, gain_ref, slots_ref,
    mid_ref, ffn_ref, out_ref, *, chunks,
):
    width = weight_ref.shape[0] // 2
    half = half_ref[0]
    squares = jnp.sum(
        own_ref[:, width:].astype(F32) + recv_ref[:, width:].astype(F32), axis=1, keepdims=True
    ) * (4.0 / LANES)
    inv_rms = lax.rsqrt(squares / (2 * width) + norm_eps)
    update = dot(own_ref[:, :width], weight_ref[pl.ds(pl.multiple_of(half * width, width), width), :])
    update = update + dot(
        recv_ref[:, :width], weight_ref[pl.ds(pl.multiple_of((1 - half) * width, width), width), :]
    )
    mid = (residual_ref[...].astype(F32) + update * inv_rms).astype(BF)
    mid_ref[...] = mid
    mid_float = mid.astype(F32)
    mid_rms = lax.rsqrt(jnp.mean(mid_float * mid_float, axis=1, keepdims=True) + norm_eps)
    ffn = (mid_float * mid_rms * gain_ref[...].astype(F32)).astype(BF)
    ffn_ref[...] = ffn
    step = slots_ref.shape[0] // chunks
    for i in range(chunks):
        at = pl.ds(i * step, step)
        out_ref[at, :] = dot(slots_ref[at, :], ffn).astype(BF)


def expert_kernel(
    x_ref, gate_ref, up_ref, down_ref, ffn_ref, mid_ref, shared_gate_ref, shared_up_ref, shared_down_ref,
    out_ref, base_ref, *, chunks,
):
    def apply(rows, gate, up, down):
        hidden = (jax.nn.silu(dot(rows, gate[...])) * dot(rows, up[...])).astype(BF)
        return dot(hidden, down[...])

    shared = apply(ffn_ref[...], shared_gate_ref, shared_up_ref, shared_down_ref)
    base_ref[...] = mid_ref[...].astype(F32) + shared
    step = x_ref.shape[0] // chunks
    for i in range(chunks):
        at = pl.ds(i * step, step)
        out_ref[at, :] = apply(x_ref[at, :], gate_ref, up_ref, down_ref).astype(BF)


def combine_kernel(mix_ref, base_ref, back_ref, out_ref, buf_ref, sems):
    rows, width = buf_ref.shape
    chunks = sems.shape[0]
    step = width // chunks
    mix = mix_ref[...]
    copies = []
    for i in range(chunks):
        at = pl.ds(i * step, step)
        both = dot(mix, back_ref[:, at])
        buf_ref[:, at] = (base_ref[:, at] + (both[:rows] + both[rows:])).astype(BF)
        copies.append(pltpu.make_async_copy(buf_ref.at[:, at], out_ref.at[:, at], sems.at[i]))
        copies[-1].start()
    for copy in copies:
        copy.wait()


def shards(
    residual, outer_gate, conv_input, conv_value, doc_ids, conv_taps, branch_gain, out_weight,
    ffn_gain, route_ids, route_weight, shared_gate, shared_up, shared_down,
    expert_gate, expert_up, expert_down,
):
    rows, width = conv_input.shape
    local, model = residual.shape
    top = route_ids.shape[1]
    peers = lax.axis_size("sp")
    cores = lax.axis_size("tp")
    experts = peers * cores
    capacity = local * cores * top // experts
    slots = experts * capacity
    wide = width + LANES
    half = lax.axis_index("tp").astype(jnp.int32).reshape(1)

    doc = doc_ids.reshape(1, rows)
    tail = pl.pallas_call(
        tail_kernel,
        out_shape=jax.ShapeDtypeStruct((24, width), BF),
        grid=(1,), name="tail",
        in_specs=[
            pl.BlockSpec((16, width), lambda i: (rows // 16 - 1, 0)),
            pl.BlockSpec((16, width), lambda i: (rows // 16 - 1, 0)),
            pl.BlockSpec((1, LANES), lambda i: (0, rows // LANES - 1)),
        ],
        out_specs=pl.BlockSpec((24, width), lambda i: (0, 0)),
        compiler_params=params(4), cost_estimate=cost(LONG, 0),
    )(*[pltpu.with_memory_space_constraint(a, pltpu.HBM) for a in (conv_input, conv_value, doc)])
    halo = lax.ppermute(tail, "sp", [(i, i + 1) for i in range(peers - 1)])

    slot_hot, mix = pl.pallas_call(
        functools.partial(slots_kernel, capacity=capacity),
        out_shape=[jax.ShapeDtypeStruct((slots, local), BF), jax.ShapeDtypeStruct((2 * local, slots), BF)],
        in_specs=[VM] * 2, out_specs=[VM] * 2, name="slots",
        compiler_params=params(6), cost_estimate=cost(SHORT, 0),
    )(route_ids.T, route_weight.T)

    halo, slot_hot, mix = lax.optimization_barrier((halo, slot_hot, mix))
    own, send = pl.pallas_call(
        conv_kernel,
        out_shape=[jax.ShapeDtypeStruct((local, wide), BF)] * 2,
        in_specs=[SM] + [VM] * 7, out_specs=[VM, VM], name="conv",
        scratch_shapes=[pltpu.VMEM((rows + 8, wide), F32), pltpu.VMEM((rows, wide), F32)],
        compiler_params=params(6), cost_estimate=cost(SHORT, 0),
    )(half, outer_gate, conv_input, conv_value, doc, halo, conv_taps, branch_gain.reshape(1, width))
    recv = lax.ppermute(send, "tp", [(0, 1), (1, 0)])

    chunks = 4
    mid, ffn, outgoing = pl.pallas_call(
        functools.partial(mid_kernel, chunks=chunks),
        out_shape=[jax.ShapeDtypeStruct((local, model), BF)] * 2 + [jax.ShapeDtypeStruct((slots, model), BF)],
        in_specs=[SM] + [VM] * 6, out_specs=[VM, VM, VM], name="mid",
        compiler_params=params(12), cost_estimate=cost(LONG, 0),
    )(half, own, recv, out_weight, residual, ffn_gain.reshape(1, model), slot_hot)

    arrived = lax.all_to_all(
        outgoing.reshape(experts, capacity, model), ("sp", "tp"), split_axis=0, concat_axis=0, tiled=True
    ).reshape(slots, model)
    result, base = pl.pallas_call(
        functools.partial(expert_kernel, chunks=chunks),
        out_shape=[jax.ShapeDtypeStruct((slots, model), BF), jax.ShapeDtypeStruct((local, model), F32)],
        in_specs=[VM] * 9, out_specs=[VM] * 2, name="expert",
        compiler_params=params(12), cost_estimate=cost(LONG, 0),
    )(arrived, expert_gate[0], expert_up[0], expert_down[0], ffn, mid, shared_gate, shared_up, shared_down)
    returned = lax.all_to_all(
        result.reshape(experts, capacity, model), ("sp", "tp"), split_axis=0, concat_axis=0, tiled=True
    ).reshape(slots, model)

    return pl.pallas_call(
        combine_kernel,
        out_shape=jax.ShapeDtypeStruct((local, model), BF),
        in_specs=[VM] * 3, out_specs=HBM, name="combine",
        scratch_shapes=[pltpu.VMEM((local, model), BF), pltpu.SemaphoreType.DMA((4,))],
        compiler_params=params(8), cost_estimate=cost(LONG, 0),
    )(mix, base, returned)


def solution(mesh):
    placed = (
        P(("sp", "tp"), None), P("sp", "tp"), P("sp", "tp"), P("sp", "tp"), P("sp"), P(None, "tp"),
        P("tp"), P(), P(), P(("sp", "tp"), None), P(("sp", "tp"), None), P(), P(), P(),
        P(("sp", "tp"), None, None), P(("sp", "tp"), None, None), P(("sp", "tp"), None, None),
    )
    return jax.shard_map(
        shards, mesh=mesh, in_specs=placed, out_specs=P(("sp", "tp"), None), check_vma=False
    )
```

```python
import functools
import jax
import jax.numpy as jnp
from jax import lax
from jax.experimental import pallas as pl
from jax.experimental.pallas import tpu as pltpu
from jax.sharding import PartitionSpec as P

norm_eps = 1e-06
BF = jnp.bfloat16
F32 = jnp.float32
MIB = 1 << 20
LANES = 128

VM = pl.BlockSpec(memory_space=pltpu.VMEM)
SM = pl.BlockSpec(memory_space=pltpu.SMEM)
HBM = pl.BlockSpec(memory_space=pltpu.HBM)
LONG = 1 << 33
SHORT = 1 << 31
LEAD = 1 << 31


def params(mib):
    return pltpu.CompilerParams(vmem_limit_bytes=mib * MIB)


def cost(flops, nbytes):
    return pl.CostEstimate(flops=flops, bytes_accessed=nbytes, transcendentals=0)


def dot(a, b):
    return jnp.dot(a, b, preferred_element_type=F32)


def tail_kernel(input_ref, value_ref, doc_ref, tail_ref):
    width = input_ref.shape[1]
    tail_ref[0:8, :] = input_ref[8:16, :]
    tail_ref[8:16, :] = value_ref[8:16, :]
    last = jnp.transpose(jnp.broadcast_to(doc_ref[...].astype(F32), (LANES, LANES)))
    tail_ref[16:24, :] = jnp.concatenate([last[LANES - 8 :, :].astype(BF)] * (width // LANES), axis=1)


def fill_slots(ids_ref, share_ref, hot_ref, mix_ref, capacity):
    slots, rows = hot_ref.shape
    slot = lax.broadcasted_iota(jnp.int32, (slots, rows), 0)
    expert = slot // capacity
    place = (slot % capacity).astype(F32)
    hit = jnp.zeros((slots, rows), F32)
    share = jnp.zeros((slots, rows), F32)
    for k in range(ids_ref.shape[0]):
        named = expert == ids_ref[k : k + 1, :]
        hit = jnp.where(named, 1.0, hit)
        share = jnp.where(named, share_ref[k : k + 1, :], share)
    before = lax.broadcasted_iota(jnp.int32, (rows, rows), 0) < lax.broadcasted_iota(
        jnp.int32, (rows, rows), 1
    )
    mine = dot(hit.astype(BF), before.astype(F32).astype(BF)) == place
    hot_ref[...] = jnp.where(mine, hit, 0.0).astype(BF)
    share = jnp.transpose(jnp.where(mine, share, 0.0))
    high = share.astype(BF)
    mix_ref[:rows, :] = high
    mix_ref[rows:, :] = (share - high.astype(F32)).astype(BF)


def convolve(gate, ext_ref, taps_ref, gain_ref):
    rows, width = gate.shape
    taps = taps_ref.shape[0]
    doc = ext_ref[8 : 8 + rows, width:]
    mixed = jnp.zeros((rows, width), F32)
    for tap in range(taps):
        start = 9 - taps + tap
        same = (ext_ref[start : start + rows, width:] == doc).astype(F32)
        same = jnp.concatenate([same] * (width // LANES), axis=1)
        mixed = mixed + taps_ref[tap : tap + 1, :].astype(F32) * ext_ref[start : start + rows, :width] * same
    branch = gate.astype(F32) * mixed
    total = jnp.broadcast_to(jnp.sum(branch * branch, axis=1, keepdims=True), (rows, LANES))
    high = total.astype(BF).astype(F32)
    middle = (total - high).astype(BF).astype(F32)
    low = total - high - middle
    part = lax.broadcasted_iota(jnp.int32, (rows, LANES), 1) % 4
    packed = jnp.where(part == 0, high, jnp.where(part == 1, middle, jnp.where(part == 2, low, 0.0)))
    return (branch * gain_ref[...].astype(F32)).astype(BF), packed.astype(BF)


def early_kernel(
    half_ref, gate_ref, input_ref, value_ref, doc_ref, taps_ref, gain_ref, ids_ref, share_ref, weight_ref,
    own_ref, send_ref, hot_ref, mix_ref, near_ref, far_ref, ext_ref, all_ref, sems, *, capacity,
):
    half = half_ref[0]
    size = near_ref.shape[0]
    copies = [
        pltpu.make_async_copy(weight_ref.at[pl.ds(pl.multiple_of(which * size, size), size), :], to, sems.at[i])
        for i, (which, to) in enumerate(((half, near_ref), (1 - half, far_ref)))
    ]
    for copy in copies:
        copy.start()
    rows, width = gate_ref.shape
    ext_ref[0:8, :] = jnp.zeros((8, width + LANES), F32)
    ext_ref[8:, :width] = input_ref[...].astype(F32) * value_ref[...].astype(F32)
    ext_ref[8:, width:] = jnp.transpose(jnp.broadcast_to(doc_ref[...].astype(F32), (LANES, rows)))
    all_ref[:, :width], all_ref[:, width:] = convolve(gate_ref[...], ext_ref, taps_ref, gain_ref)
    local = rows // 2
    own_ref[...] = all_ref[pl.ds(pl.multiple_of(half * local, local), local), :]
    send_ref[...] = all_ref[pl.ds(pl.multiple_of((1 - half) * local, local), local), :]
    fill_slots(ids_ref, share_ref, hot_ref, mix_ref, capacity)
    for copy in copies:
        copy.wait()


def lead_kernel(
    half_ref, own_in_ref, send_in_ref, gate_ref, input_ref, value_ref, doc_ref, halo_ref, taps_ref, gain_ref,
    own_ref, send_ref, ext_ref,
):
    width = gate_ref.shape[1]
    ext_ref[0:8, :width] = halo_ref[0:8, :].astype(F32) * halo_ref[8:16, :].astype(F32)
    ext_ref[0:8, width:] = halo_ref[16:24, :LANES].astype(F32)
    ext_ref[8:24, :width] = input_ref[0:16, :].astype(F32) * value_ref[0:16, :].astype(F32)
    doc = jnp.transpose(jnp.broadcast_to(doc_ref[:, :LANES].astype(F32), (LANES, LANES)))
    ext_ref[8:24, width:] = doc[0:16, :]
    scaled, packed = convolve(gate_ref[0:16, :], ext_ref, taps_ref, gain_ref)
    own_ref[...] = own_in_ref[...]
    send_ref[...] = send_in_ref[...]

    @pl.when(half_ref[0] == 0)
    def _():
        own_ref[0:16, :width] = scaled
        own_ref[0:16, width:] = packed

    @pl.when(half_ref[0] == 1)
    def _():
        send_ref[0:16, :width] = scaled
        send_ref[0:16, width:] = packed


def half_kernel(own_ref, near_ref, part_ref):
    part_ref[...] = dot(own_ref[:, : near_ref.shape[0]], near_ref[...])


def mid_kernel(
    own_ref, recv_ref, part_ref, far_ref, residual_ref, gain_ref, slots_ref,
    mid_ref, ffn_ref, out_ref, *, chunks,
):
    width = far_ref.shape[0]
    squares = jnp.sum(
        own_ref[:, width:].astype(F32) + recv_ref[:, width:].astype(F32), axis=1, keepdims=True
    ) * (4.0 / LANES)
    inv_rms = lax.rsqrt(squares / (2 * width) + norm_eps)
    update = part_ref[...] + dot(recv_ref[:, :width], far_ref[...])
    mid = (residual_ref[...].astype(F32) + update * inv_rms).astype(BF)
    mid_ref[...] = mid
    mid_float = mid.astype(F32)
    mid_rms = lax.rsqrt(jnp.mean(mid_float * mid_float, axis=1, keepdims=True) + norm_eps)
    ffn = (mid_float * mid_rms * gain_ref[...].astype(F32)).astype(BF)
    ffn_ref[...] = ffn
    step = slots_ref.shape[0] // chunks
    for i in range(chunks):
        at = pl.ds(i * step, step)
        out_ref[at, :] = dot(slots_ref[at, :], ffn).astype(BF)


def expert_kernel(
    x_ref, gate_ref, up_ref, down_ref, ffn_ref, mid_ref, shared_gate_ref, shared_up_ref, shared_down_ref,
    out_ref, base_ref, *, chunks,
):
    def apply(rows, gate, up, down):
        hidden = (jax.nn.silu(dot(rows, gate[...])) * dot(rows, up[...])).astype(BF)
        return dot(hidden, down[...])

    shared = apply(ffn_ref[...], shared_gate_ref, shared_up_ref, shared_down_ref)
    base_ref[...] = mid_ref[...].astype(F32) + shared
    step = x_ref.shape[0] // chunks
    for i in range(chunks):
        at = pl.ds(i * step, step)
        out_ref[at, :] = apply(x_ref[at, :], gate_ref, up_ref, down_ref).astype(BF)


def combine_kernel(mix_ref, base_ref, back_ref, out_ref, buf_ref, sems):
    rows, width = buf_ref.shape
    chunks = sems.shape[0]
    step = width // chunks
    mix = mix_ref[...]
    copies = []
    for i in range(chunks):
        at = pl.ds(i * step, step)
        both = dot(mix, back_ref[:, at])
        buf_ref[:, at] = (base_ref[:, at] + (both[:rows] + both[rows:])).astype(BF)
        copies.append(pltpu.make_async_copy(buf_ref.at[:, at], out_ref.at[:, at], sems.at[i]))
        copies[-1].start()
    for copy in copies:
        copy.wait()


def shards(
    residual, outer_gate, conv_input, conv_value, doc_ids, conv_taps, branch_gain, out_weight,
    ffn_gain, route_ids, route_weight, shared_gate, shared_up, shared_down,
    expert_gate, expert_up, expert_down,
):
    rows, width = conv_input.shape
    local, model = residual.shape
    top = route_ids.shape[1]
    peers = lax.axis_size("sp")
    cores = lax.axis_size("tp")
    experts = peers * cores
    capacity = local * cores * top // experts
    slots = experts * capacity
    wide = width + LANES
    half = lax.axis_index("tp").astype(jnp.int32).reshape(1)

    doc = doc_ids.reshape(1, rows)
    tail = pl.pallas_call(
        tail_kernel,
        out_shape=jax.ShapeDtypeStruct((24, width), BF),
        grid=(1,), name="tail",
        in_specs=[
            pl.BlockSpec((16, width), lambda i: (rows // 16 - 1, 0)),
            pl.BlockSpec((16, width), lambda i: (rows // 16 - 1, 0)),
            pl.BlockSpec((1, LANES), lambda i: (0, rows // LANES - 1)),
        ],
        out_specs=pl.BlockSpec((24, width), lambda i: (0, 0)),
        compiler_params=params(4), cost_estimate=cost(LONG, 0),
    )(*[pltpu.with_memory_space_constraint(a, pltpu.HBM) for a in (conv_input, conv_value, doc)])
    halo = lax.ppermute(tail, "sp", [(i, i + 1) for i in range(peers - 1)])

    gain = branch_gain.reshape(1, width)
    mover = jax.ShapeDtypeStruct((local, wide), BF)
    piece = jax.ShapeDtypeStruct((width, model), BF)
    own, send, slot_hot, mix, near, far = pl.pallas_call(
        functools.partial(early_kernel, capacity=capacity),
        out_shape=[
            mover, mover, jax.ShapeDtypeStruct((slots, local), BF), jax.ShapeDtypeStruct((2 * local, slots), BF),
            piece, piece,
        ],
        in_specs=[SM] + [VM] * 8 + [HBM], out_specs=[VM] * 6, name="early",
        scratch_shapes=[
            pltpu.VMEM((rows + 8, wide), F32), pltpu.VMEM((rows, wide), BF), pltpu.SemaphoreType.DMA((2,)),
        ],
        compiler_params=params(12), cost_estimate=cost(SHORT, 0),
    )(
        half, outer_gate, conv_input, conv_value, doc, conv_taps, gain, route_ids.T, route_weight.T,
        pltpu.with_memory_space_constraint(out_weight, pltpu.HBM),
    )
    halo, own, send = lax.optimization_barrier((halo, own, send))
    own, send = pl.pallas_call(
        lead_kernel,
        out_shape=[mover, mover],
        in_specs=[SM] + [VM] * 9, out_specs=[VM, VM], name="lead",
        scratch_shapes=[pltpu.VMEM((24, wide), F32)],
        compiler_params=params(6), cost_estimate=cost(LEAD, 0),
    )(half, own, send, outer_gate, conv_input, conv_value, doc, halo, conv_taps, gain)
    recv = lax.ppermute(send, "tp", [(0, 1), (1, 0)])
    part = pl.pallas_call(
        half_kernel,
        out_shape=jax.ShapeDtypeStruct((local, model), F32),
        in_specs=[VM, VM], out_specs=VM, name="half",
        compiler_params=params(6), cost_estimate=cost(LEAD, 0),
    )(own, near)

    chunks = 4
    mid, ffn, outgoing = pl.pallas_call(
        functools.partial(mid_kernel, chunks=chunks),
        out_shape=[jax.ShapeDtypeStruct((local, model), BF)] * 2 + [jax.ShapeDtypeStruct((slots, model), BF)],
        in_specs=[VM] * 7, out_specs=[VM, VM, VM], name="mid",
        compiler_params=params(12), cost_estimate=cost(LONG, 0),
    )(own, recv, part, far, residual, ffn_gain.reshape(1, model), slot_hot)

    arrived = lax.all_to_all(
        outgoing.reshape(experts, capacity, model), ("sp", "tp"), split_axis=0, concat_axis=0, tiled=True
    ).reshape(slots, model)
    result, base = pl.pallas_call(
        functools.partial(expert_kernel, chunks=chunks),
        out_shape=[jax.ShapeDtypeStruct((slots, model), BF), jax.ShapeDtypeStruct((local, model), F32)],
        in_specs=[VM] * 9, out_specs=[VM] * 2, name="expert",
        compiler_params=params(12), cost_estimate=cost(LONG, 0),
    )(arrived, expert_gate[0], expert_up[0], expert_down[0], ffn, mid, shared_gate, shared_up, shared_down)
    returned = lax.all_to_all(
        result.reshape(experts, capacity, model), ("sp", "tp"), split_axis=0, concat_axis=0, tiled=True
    ).reshape(slots, model)

    return pl.pallas_call(
        combine_kernel,
        out_shape=jax.ShapeDtypeStruct((local, model), BF),
        in_specs=[VM] * 3, out_specs=HBM, name="combine",
        scratch_shapes=[pltpu.VMEM((local, model), BF), pltpu.SemaphoreType.DMA((4,))],
        compiler_params=params(8), cost_estimate=cost(LONG, 0),
    )(mix, base, returned)


def solution(mesh):
    placed = (
        P(("sp", "tp"), None), P("sp", "tp"), P("sp", "tp"), P("sp", "tp"), P("sp"), P(None, "tp"),
        P("tp"), P(), P(), P(("sp", "tp"), None), P(("sp", "tp"), None), P(), P(), P(),
        P(("sp", "tp"), None, None), P(("sp", "tp"), None, None), P(("sp", "tp"), None, None),
    )
    return jax.shard_map(
        shards, mesh=mesh, in_specs=placed, out_specs=P(("sp", "tp"), None), check_vma=False
    )
```
